32 devices in a mesh: sp: 4 (over z), fs: 4 (over y, x), tp: 2 (over core).
Axes of the slice: x: 2, y: 2, z: 4, core: 2. Of those that a mesh axis runs over, the one named last changes fastest.
Arguments:
- tokens: bfloat16 [8192, 2048], P(('fs', 'sp')), parts along dimension 0, may hold values from -6 to 6
- norm_gain: float32 [2048], replicated, may hold values from 0.1 to 1.9
- state_gate: bfloat16 [2048, 1024], P('sp', 'tp'), may hold values from -0.125 to 0.125
- state_value: bfloat16 [2048, 1024], P('sp', 'tp'), may hold values from -0.125 to 0.125
- state_keys: bfloat16 [2048, 1024], P('sp', 'tp'), may hold values from -0.125 to 0.125
- state_query: bfloat16 [2048, 1024], P('sp', 'tp'), may hold values from -0.125 to 0.125
- state_step: bfloat16 [2048, 16], replicated, may hold values from -0.125 to 0.125
- state_rate: float32 [16], P('tp'), may hold values from 0 to 1, as said below
- state_jumps: float32 [8192, 16], P(('fs', 'sp'), 'tp'), parts along dimension 0, may hold values from -3 to 0
- state_gain: float32 [1024], P('tp'), may hold values from 0.1 to 1.9
- filter_value: bfloat16 [5, 1024], P(None, 'tp'), may hold values from -2.5 to 2.5
- filter_keys: bfloat16 [5, 1024], P(None, 'tp'), may hold values from -2.5 to 2.5
- filter_query: bfloat16 [5, 1024], P(None, 'tp'), may hold values from -2.5 to 2.5
- window_query: bfloat16 [2048, 2048], P('sp', 'tp'), may hold values from -64 to 64
- window_keys: bfloat16 [2048, 1024], P('sp', 'tp'), may hold values from -1 to 1
- window_values: bfloat16 [2048, 1024], P('sp', 'tp'), may hold values from -0.125 to 0.125
- window_sink: float32 [16], P('tp'), may hold values from 2.5 to 5.5
- state_output: bfloat16 [1024, 2048], P('tp', 'sp'), may hold values from -0.1875 to 0.1875
- window_output: bfloat16 [2048, 2048], P('tp', 'sp'), may hold values from -2 to 2
Outputs:
- mixed: bfloat16 [8192, 2048], P(('fs', 'sp', 'tp')), parts along dimension 0
The draws below stay inside these ranges and needn't reach their ends.
There are 4 independent parts, one for each index of `fs`. The reference program is written for one: setup_inputs(seed, part) draws one part's arguments, and reference() takes and returns one part's arrays. A program takes and returns all parts, laid end to end along the dimension named above; an argument that names none is the same for every part. Nothing has to cross between parts.
Inputs may be any that keep to these rules, and one draw needn't show every extreme that they name: `state_rate`: a positive rate for each head.
All inputs are finite; a program needn't handle non-finite values.
Results may differ from the reference program's by a relative error of at most 0.015.
The reference program's roundings to bfloat16 on the way count: a program that leaves them out, or rounds other values in their place, can miss the bound.
Values may be sent and summed in bfloat16 or wider, within the bound.
A program may use at most 64 MiB of HBM per device.

```python
import math
import jax
import jax.numpy as jnp
from jax import lax

D = 2048
MIXER_STATE_HEADS = 16
STATE_HEAD_DIM = 64
STATE_GROUPS = 8
STATE_SIZE = 128
WINDOW_HEADS = 16
WINDOW_KV_HEADS = 8
HEAD_DIM = 128
CONV_WIDTH = 5
WINDOW = 128
BLOCK = 128
GRID_WIDTH = 64
TOK_DEV = 512
SEQUENCE_LENGTH = 2048
STATE_INNER = 1024
GROUP_WIDTH = 1024
WINDOW_WIDTH = 2048
KV_WIDTH = 1024
N_TP = 2


def draw_state_rate(key, part):
    shuffled = jax.random.permutation(jax.random.fold_in(key, 101), MIXER_STATE_HEADS)
    quick_count = MIXER_STATE_HEADS // 2
    quick_heads = shuffled < quick_count
    quick_rate = jnp.exp(jax.random.uniform(jax.random.fold_in(key, 102), (MIXER_STATE_HEADS,), jnp.float32, math.log(1.0 / 60.0), math.log(1.0 / 20.0)))
    slow_rate = jax.random.uniform(jax.random.fold_in(key, 103), (MIXER_STATE_HEADS,), jnp.float32, 0.1, 0.4) / SEQUENCE_LENGTH
    return jnp.where(quick_heads, quick_rate, slow_rate).astype(jnp.float32)


def draw_state_jumps(key, part):
    block_count = SEQUENCE_LENGTH // TOK_DEV
    factors = jnp.exp(jax.random.uniform(jax.random.fold_in(key, 201), (block_count,), jnp.float32, math.log(0.5), math.log(2.5)))
    token_position = jnp.arange(SEQUENCE_LENGTH)
    baseline_level = -0.3 * jnp.take(factors, token_position // TOK_DEV) / SEQUENCE_LENGTH
    spike_positions = jax.random.randint(jax.random.fold_in(key, 202), (3,), 0, SEQUENCE_LENGTH)
    spike_count = (token_position[None, :] == spike_positions[:, None]).astype(jnp.float32)
    spike_depth = jnp.log(jax.random.uniform(jax.random.fold_in(key, 203), (3, MIXER_STATE_HEADS), jnp.float32, 0.5, 0.8))
    return (baseline_level[:, None] + jnp.dot(spike_count.T, spike_depth)).astype(jnp.float32)


def draw_tokens(key, part):
    rows = jnp.clip(jax.random.normal(jax.random.fold_in(key, 404), (SEQUENCE_LENGTH, D), jnp.float32), -6.0, 6.0)
    return rows.astype(jnp.bfloat16)


def window_pair(key):
    scale = 1.0 / math.sqrt(D)
    keys_all = jnp.clip(jax.random.normal(jax.random.fold_in(key, 306), (D, KV_WIDTH), jnp.float32), -6.0, 6.0) * scale
    query_all = jnp.clip(jax.random.normal(jax.random.fold_in(key, 307), (D, WINDOW_WIDTH), jnp.float32), -6.0, 6.0) * scale
    return (query_all.astype(jnp.float32), keys_all.astype(jnp.float32))


def draw_window_query(key, part):
    return window_pair(key)[0].astype(jnp.bfloat16)


def draw_window_keys(key, part):
    return window_pair(key)[1].astype(jnp.bfloat16)


def levels(rng, shape, split, smallest, top_value):
    def one(dim, parts):
        heights = jax.random.uniform(jax.random.fold_in(jax.random.fold_in(rng, 6), dim), (parts,), jnp.float32, smallest / len(split), top_value / len(split))
        return jnp.repeat(jnp.exp(heights), shape[dim] // parts).reshape((-1,) + (1,) * (len(shape) - dim - 1))

    factor_of = one(*split[0])
    for cut in split[1:]:
        factor_of = factor_of * one(*cut)
    return factor_of


def centred(rng, shape, scale, reach, cuts=(), kind=jnp.bfloat16):
    result = scale * jax.random.normal(rng, shape, jnp.float32)
    if cuts:
        result = result * levels(rng, shape, cuts, -0.22, 0.18)
    return jnp.clip(result, -reach, reach).astype(kind)


def setup_inputs(seed: int = 0, part: int = 0) -> dict:
    key_list = jax.random.split(jax.random.key(seed), 20)
    part_splits = jax.random.split(jax.random.fold_in(key_list[19], part), 20)
    return {
        "tokens": draw_tokens(jax.random.fold_in(jax.random.fold_in(key_list[19], part), 71), part),
        "norm_gain": jnp.clip(1.0 + 0.18 * jax.random.normal(key_list[1], (D,), jnp.float32), 0.1, 1.9),
        "state_gate": centred(key_list[2], (D, STATE_INNER), D ** -0.5, 0.125, ((0, 4), (1, 2))),
        "state_value": centred(key_list[3], (D, STATE_INNER), D ** -0.5, 0.125, ((0, 4), (1, 2))),
        "state_keys": centred(key_list[4], (D, GROUP_WIDTH), D ** -0.5, 0.125, ((0, 4), (1, 2))),
        "state_query": centred(key_list[5], (D, GROUP_WIDTH), D ** -0.5, 0.125, ((0, 4), (1, 2))),
        "state_step": centred(key_list[6], (D, MIXER_STATE_HEADS), D ** -0.5, 0.125),
        "state_rate": draw_state_rate(jax.random.fold_in(key_list[19], 71), part),
        "state_jumps": draw_state_jumps(jax.random.fold_in(jax.random.fold_in(key_list[19], part), 71), part),
        "state_gain": jnp.clip(1.0 + 0.18 * jax.random.normal(key_list[9], (STATE_INNER,), jnp.float32), 0.1, 1.9),
        "filter_value": centred(key_list[10], (CONV_WIDTH, STATE_INNER), CONV_WIDTH ** -0.5, 2.5, ((1, 2),)),
        "filter_keys": centred(key_list[11], (CONV_WIDTH, GROUP_WIDTH), CONV_WIDTH ** -0.5, 2.5, ((1, 2),)),
        "filter_query": centred(key_list[12], (CONV_WIDTH, GROUP_WIDTH), CONV_WIDTH ** -0.5, 2.5, ((1, 2),)),
        "window_query": draw_window_query(jax.random.fold_in(key_list[19], 71), part),
        "window_keys": draw_window_keys(jax.random.fold_in(key_list[19], 71), part),
        "window_values": centred(key_list[15], (D, KV_WIDTH), D ** -0.5, 0.125, ((0, 4), (1, 2))),
        "window_sink": jnp.clip(2.5 + 3.0 * jax.random.uniform(key_list[16], (WINDOW_HEADS,), jnp.float32) ** levels(key_list[16], (WINDOW_HEADS,), ((0, 2),), -0.2, 0.2), 2.5, 5.5),
        "state_output": centred(key_list[17], (STATE_INNER, D), STATE_INNER ** -0.5, 0.1875, ((0, 2), (1, 4))),
        "window_output": centred(key_list[18], (WINDOW_WIDTH, D), (WINDOW_WIDTH // (2 * WINDOW + 1)) ** -0.5, 2.0, ((0, 2), (1, 4))),
    }


def rotate_grid(vectors, positions, grid_width):
    head_dim = vectors.shape[-1]
    quarter = head_dim // 4
    half_dim = head_dim // 2
    inverse = 10000.0 ** (-jnp.arange(quarter, dtype=jnp.float32) / quarter)
    grid_row = (positions // grid_width).astype(jnp.float32)
    grid_col = (positions % grid_width).astype(jnp.float32)
    angle_row = grid_row[:, None] * inverse[None, :]
    angle_col = grid_col[:, None] * inverse[None, :]
    angles = jnp.concatenate([angle_row, angle_row, angle_col, angle_col], axis=-1)[:, None, :]
    first_half = vectors[..., :half_dim]
    second = vectors[..., half_dim:]
    turned = jnp.concatenate([-first_half[..., quarter:], first_half[..., :quarter], -second[..., quarter:], second[..., :quarter]], axis=-1)
    return (vectors.astype(jnp.float32) * jnp.cos(angles) + turned.astype(jnp.float32) * jnp.sin(angles)).astype(jnp.bfloat16)

def window_attend(query_rows, keys_pad, values_pad, sink_logits, key_start, total_len, window):
    row_count, query_heads, head_dim = query_rows.shape
    kv_heads = keys_pad.shape[1]
    group_size = query_heads // kv_heads
    block_count = row_count // window
    query_blocks = query_rows.reshape(block_count, window, kv_heads, group_size, head_dim)
    key_split = keys_pad.reshape(block_count + 2, window, kv_heads, head_dim)
    value_split = values_pad.reshape(block_count + 2, window, kv_heads, head_dim)
    key_band = jnp.concatenate([key_split[:-2], key_split[1:-1], key_split[2:]], axis=1)
    value_band = jnp.concatenate([value_split[:-2], value_split[1:-1], value_split[2:]], axis=1)
    scores = jnp.einsum('kihgd,kjhd->khgij', query_blocks.astype(jnp.float32), key_band.astype(jnp.float32)) * head_dim ** (-0.5)
    query_pos = jnp.arange(window)[:, None]
    band_pos = jnp.arange(3 * window)[None, :]
    within = jnp.abs(band_pos - window - query_pos) <= window
    key_pos = key_start + jnp.arange(block_count)[:, None] * window + jnp.arange(3 * window)[None, :]
    inside = (key_pos >= 0) & (key_pos < total_len)
    valid_pair = (within[None] & inside[:, None, :])[:, None, None]
    sink_logit = sink_logits.reshape(kv_heads, group_size)[None, :, :, None, None]
    masked = jnp.where(valid_pair, scores, -1e+30)
    ceiling = jnp.maximum(lax.optimization_barrier(jnp.max(masked, axis=-1, keepdims=True)), sink_logit)
    weights = jnp.where(valid_pair, jnp.exp(masked - ceiling), 0.0)
    denominator = jnp.exp(sink_logit - ceiling) + lax.optimization_barrier(jnp.sum(weights, axis=-1, keepdims=True))
    weights_bf = (weights / denominator).astype(jnp.bfloat16)
    mixed_rows = jnp.einsum('khgij,kjhd->kihgd', weights_bf.astype(jnp.float32), value_band.astype(jnp.float32))
    return mixed_rows.reshape(row_count, query_heads * head_dim).astype(jnp.bfloat16)

def block_terms(query_rows, key_rows, value_rows, log_rows, block_len):
    row_count, group_count, state_size = query_rows.shape
    head_ratio, head_dim = (value_rows.shape[2], value_rows.shape[3])
    block_count = row_count // block_len
    query_blocks = query_rows.reshape(block_count, block_len, group_count, state_size)
    key_blocks = key_rows.reshape(block_count, block_len, group_count, state_size)
    value_blocks = value_rows.reshape(block_count, block_len, group_count, head_ratio, head_dim)
    decay_cum = jnp.cumsum(log_rows.reshape(block_count, block_len, group_count, head_ratio), axis=1)
    decay_total = decay_cum[:, -1]
    gram_block = jnp.einsum('kign,kjgn->kgij', query_blocks.astype(jnp.float32), key_blocks.astype(jnp.float32))
    cum_heads = jnp.moveaxis(decay_cum, 1, 3)
    distance = jnp.abs(cum_heads[..., :, None] - cum_heads[..., None, :])
    pair_weight = (gram_block[:, :, None] * jnp.exp(-distance)).astype(jnp.bfloat16)
    near_terms = jnp.einsum('kgrij,kjgrp->kigrp', pair_weight.astype(jnp.float32), value_blocks.astype(jnp.float32))
    keys_after = (key_blocks[:, :, :, None, :] * jnp.exp(decay_total[:, None] - decay_cum)[..., None]).astype(jnp.bfloat16)
    keys_before = (key_blocks[:, :, :, None, :] * jnp.exp(decay_cum)[..., None]).astype(jnp.bfloat16)
    state_after = jnp.einsum('kjgrn,kjgrp->kgrnp', keys_after.astype(jnp.float32), value_blocks.astype(jnp.float32))
    state_before = jnp.einsum('kjgrn,kjgrp->kgrnp', keys_before.astype(jnp.float32), value_blocks.astype(jnp.float32))
    before = jnp.cumsum(decay_total, axis=0) - decay_total
    overall = lax.optimization_barrier(jnp.sum(decay_total, axis=0))
    after_sum = overall[None] - before - decay_total
    block_order = jnp.arange(block_count)
    earlier_mask = (block_order[None, :] < block_order[:, None])[:, :, None, None]
    later_mask = (block_order[None, :] > block_order[:, None])[:, :, None, None]
    gap_fwd = before[:, None] - before[None, :] - decay_total[None, :]
    gap_bwd = before[None, :] - before[:, None] - decay_total[:, None]
    weight_fwd = jnp.where(earlier_mask, jnp.exp(jnp.minimum(gap_fwd, 0.0)), 0.0)
    weight_bwd = jnp.where(later_mask, jnp.exp(jnp.minimum(gap_bwd, 0.0)), 0.0)
    carried_fwd = jnp.einsum('abgr,bgrnp->agrnp', weight_fwd, state_after, precision=lax.Precision.HIGHEST)
    carried_bwd = jnp.einsum('abgr,bgrnp->agrnp', weight_bwd, state_before, precision=lax.Precision.HIGHEST)
    summary_fwd = jnp.einsum('agr,agrnp->grnp', jnp.exp(after_sum), state_after, precision=lax.Precision.HIGHEST)
    summary_bwd = jnp.einsum('agr,agrnp->grnp', jnp.exp(before), state_before, precision=lax.Precision.HIGHEST)
    pieces = (near_terms, carried_fwd, carried_bwd, decay_cum, decay_total, before, after_sum, query_blocks)
    return (pieces, (summary_fwd, summary_bwd, overall))

def finish_terms(pieces, incoming_fwd, incoming_bwd):
    near_terms, carried_fwd, carried_bwd, decay_cum, decay_total, before, after_sum, query_blocks = pieces
    total_fwd = carried_fwd + jnp.exp(before)[..., None, None] * incoming_fwd[None]
    total_bwd = carried_bwd + jnp.exp(after_sum)[..., None, None] * incoming_bwd[None]
    query_wide = query_blocks.astype(jnp.float32)
    read_fwd = jnp.einsum('kign,kgrnp->kigrp', query_wide, total_fwd, precision=lax.Precision.HIGHEST)
    read_bwd = jnp.einsum('kign,kgrnp->kigrp', query_wide, total_bwd, precision=lax.Precision.HIGHEST)
    combined = near_terms + jnp.exp(decay_cum)[..., None] * read_fwd + jnp.exp(decay_total[:, None] - decay_cum)[..., None] * read_bwd
    block_count, block_len, group_count, head_ratio, head_dim = combined.shape
    return combined.reshape(block_count * block_len, group_count, head_ratio, head_dim)

def reference(tokens, norm_gain, state_gate, state_value, state_keys, state_query, state_step, state_rate, state_jumps, state_gain, filter_value, filter_keys, filter_query, window_query, window_keys, window_values, window_sink, state_output, window_output):
    length, feat_width = tokens.shape
    rows_wide = tokens.astype(jnp.float32)
    normed = (rows_wide * lax.rsqrt(lax.optimization_barrier(jnp.mean(rows_wide * rows_wide, axis=-1, keepdims=True)) + 1e-06) * norm_gain).astype(jnp.bfloat16)
    gate_rows = jnp.dot(normed, state_gate, preferred_element_type=jnp.float32).astype(jnp.bfloat16)
    value_pre = jnp.dot(normed, state_value, preferred_element_type=jnp.float32).astype(jnp.bfloat16)
    keys_pre = jnp.dot(normed, state_keys, preferred_element_type=jnp.float32).astype(jnp.bfloat16)
    query_pre = jnp.dot(normed, state_query, preferred_element_type=jnp.float32).astype(jnp.bfloat16)
    query_raw = jnp.dot(normed, window_query, preferred_element_type=jnp.float32).astype(jnp.bfloat16)
    keys_raw = jnp.dot(normed, window_keys, preferred_element_type=jnp.float32).astype(jnp.bfloat16)
    values_rows = jnp.dot(normed, window_values, preferred_element_type=jnp.float32).astype(jnp.bfloat16)
    step_rows = jax.nn.softplus(jnp.dot(normed, state_step, preferred_element_type=jnp.float32))
    log_decay = -state_rate[None, :] * step_rows + state_jumps
    half_width = filter_value.shape[0] // 2
    stacked = jnp.concatenate([value_pre, keys_pre, query_pre], axis=-1)
    padded = jnp.pad(stacked, ((half_width, half_width), (0, 0)))
    filters = jnp.concatenate([filter_value, filter_keys, filter_query], axis=-1).astype(jnp.float32)
    filtered = jnp.zeros(stacked.shape, jnp.float32)
    for offset in range(filters.shape[0]):
        filtered = filtered + padded[offset:offset + length].astype(jnp.float32) * filters[offset]
    value_cols = STATE_INNER
    key_cols = GROUP_WIDTH
    head_ratio = MIXER_STATE_HEADS // STATE_GROUPS
    inner_rows = jax.nn.silu(filtered[:, :value_cols]).reshape(length, MIXER_STATE_HEADS, STATE_HEAD_DIM) * step_rows[..., None]
    scan_values = inner_rows.astype(jnp.bfloat16).reshape(length, STATE_GROUPS, head_ratio, STATE_HEAD_DIM)
    scan_keys = filtered[:, value_cols:value_cols + key_cols].astype(jnp.bfloat16).reshape(length, STATE_GROUPS, STATE_SIZE)
    scan_query = filtered[:, value_cols + key_cols:].astype(jnp.bfloat16).reshape(length, STATE_GROUPS, STATE_SIZE)
    group_logs = log_decay.reshape(length, STATE_GROUPS, head_ratio)

    def one_group(group_args):
        group_query, group_keys, group_values, group_decay = group_args
        pieces, summaries = block_terms(group_query[:, None], group_keys[:, None], group_values[:, None], group_decay[:, None], BLOCK)
        zero_state = jnp.zeros((1, head_ratio, STATE_SIZE, STATE_HEAD_DIM), jnp.float32)
        return finish_terms(pieces, zero_state, zero_state)[:, 0]
    per_group = lax.map(one_group, (jnp.moveaxis(scan_query, 1, 0), jnp.moveaxis(scan_keys, 1, 0), jnp.moveaxis(scan_values, 1, 0), jnp.moveaxis(group_logs, 1, 0)))
    scan_out = jnp.moveaxis(per_group, 0, 1).reshape(length, STATE_INNER)
    gated_rows = scan_out * jax.nn.silu(gate_rows.astype(jnp.float32))
    per_head = gated_rows.reshape(length, MIXER_STATE_HEADS, STATE_HEAD_DIM)
    state_mix = (per_head * lax.rsqrt(lax.optimization_barrier(jnp.mean(per_head * per_head, axis=-1, keepdims=True)) + 1e-06) * state_gain.reshape(MIXER_STATE_HEADS, STATE_HEAD_DIM)).astype(jnp.bfloat16).reshape(length, STATE_INNER)
    positions = jnp.arange(length, dtype=jnp.int32)
    query_rot = rotate_grid(query_raw.reshape(length, WINDOW_HEADS, HEAD_DIM), positions, GRID_WIDTH)
    keys_rot = rotate_grid(keys_raw.reshape(length, WINDOW_KV_HEADS, HEAD_DIM), positions, GRID_WIDTH)
    keys_pad = jnp.pad(keys_rot, ((WINDOW, WINDOW), (0, 0), (0, 0)))
    values_pad = jnp.pad(values_rows.reshape(length, WINDOW_KV_HEADS, HEAD_DIM), ((WINDOW, WINDOW), (0, 0), (0, 0)))
    group_size = WINDOW_HEADS // WINDOW_KV_HEADS

    def one_head(head_args):
        head_query, head_keys, head_values, head_sink = head_args
        return window_attend(head_query, head_keys[:, None], head_values[:, None], head_sink, -WINDOW, length, WINDOW)
    per_kv = lax.map(one_head, (jnp.moveaxis(query_rot.reshape(length, WINDOW_KV_HEADS, group_size, HEAD_DIM), 1, 0), jnp.moveaxis(keys_pad, 1, 0), jnp.moveaxis(values_pad, 1, 0), window_sink.reshape(WINDOW_KV_HEADS, group_size)))
    window_mix = jnp.moveaxis(per_kv, 0, 1).reshape(length, WINDOW_WIDTH)
    state_cols = STATE_INNER // N_TP
    window_cols = WINDOW_WIDTH // N_TP

    def add_group(group_index, running):
        state_start = (group_index * state_cols).astype(jnp.int32)
        window_start = (group_index * window_cols).astype(jnp.int32)
        state_part = lax.dynamic_slice_in_dim(state_mix, state_start, state_cols, 1)
        state_weight = lax.dynamic_slice_in_dim(state_output, state_start, state_cols, 0)
        window_part = lax.dynamic_slice_in_dim(window_mix, window_start, window_cols, 1)
        window_weight = lax.dynamic_slice_in_dim(window_output, window_start, window_cols, 0)
        term_rows = jnp.dot(state_part, state_weight, preferred_element_type=jnp.float32) + jnp.dot(window_part, window_weight, preferred_element_type=jnp.float32)
        rounded = lax.optimization_barrier(term_rows.astype(jnp.bfloat16))
        return running + rounded.astype(jnp.float32)
    summed = lax.fori_loop(0, N_TP, add_group, jnp.zeros((length, feat_width), jnp.float32))
    return summed.astype(jnp.bfloat16)
```

```python
import functools

import jax
import jax.numpy as jnp
from jax import lax
from jax.experimental import pallas as pl
from jax.experimental.pallas import tpu as pltpu
from jax.sharding import PartitionSpec as P

STATE_SIZE = 128
HEAD_DIM = 128
WINDOW = 128
BLOCK = 128
GRID_WIDTH = 64


def extended(cells, sides, width):
    for axis, dim in sides:
        count = lax.axis_size(axis)
        ends = count - 1
        head = lax.slice_in_dim(cells, 0, width, axis=dim)
        tail = lax.slice_in_dim(cells, cells.shape[dim] - width, cells.shape[dim], axis=dim)
        cells = jnp.concatenate(
            [
                lax.ppermute(tail, axis, [(i, (i + 1) % count) for i in range(ends)]),
                cells,
                lax.ppermute(head, axis, [((i + 1) % count, i) for i in range(ends)]),
            ],
            axis=dim,
        )
    return cells


def rotate_grid(vectors, positions, grid_width):
    head_dim = vectors.shape[-1]
    quarter = head_dim // 4
    half_dim = head_dim // 2
    inverse = 10000.0 ** (-jnp.arange(quarter, dtype=jnp.float32) / quarter)
    grid_row = (positions // grid_width).astype(jnp.float32)
    grid_col = (positions % grid_width).astype(jnp.float32)
    angle_row = grid_row[:, None] * inverse[None, :]
    angle_col = grid_col[:, None] * inverse[None, :]
    angles = jnp.concatenate([angle_row, angle_row, angle_col, angle_col], axis=-1)[:, None, :]
    first_half = vectors[..., :half_dim]
    second = vectors[..., half_dim:]
    turned = jnp.concatenate(
        [
            -first_half[..., quarter:],
            first_half[..., :quarter],
            -second[..., quarter:],
            second[..., :quarter],
        ],
        axis=-1,
    )
    return (
        vectors.astype(jnp.float32) * jnp.cos(angles) + turned.astype(jnp.float32) * jnp.sin(angles)
    ).astype(jnp.bfloat16)


def window_attend(query_rows, keys_pad, values_pad, sink_logits, key_start, total_len, window):
    row_count, query_heads, head_dim = query_rows.shape
    kv_heads = keys_pad.shape[1]
    group_size = query_heads // kv_heads
    block_count = row_count // window
    query_blocks = query_rows.reshape(block_count, window, kv_heads, group_size, head_dim)
    key_split = keys_pad.reshape(block_count + 2, window, kv_heads, head_dim)
    value_split = values_pad.reshape(block_count + 2, window, kv_heads, head_dim)
    key_band = jnp.concatenate([key_split[:-2], key_split[1:-1], key_split[2:]], axis=1)
    value_band = jnp.concatenate([value_split[:-2], value_split[1:-1], value_split[2:]], axis=1)
    scores = jnp.einsum(
        "kihgd,kjhd->khgij", query_blocks, key_band, preferred_element_type=jnp.float32
    ) * head_dim ** (-0.5)
    query_pos = jnp.arange(window)[:, None]
    band_pos = jnp.arange(3 * window)[None, :]
    within = jnp.abs(band_pos - window - query_pos) <= window
    key_pos = (
        key_start + jnp.arange(block_count)[:, None] * window + jnp.arange(3 * window)[None, :]
    )
    inside = (key_pos >= 0) & (key_pos < total_len)
    valid_pair = (within[None] & inside[:, None, :])[:, None, None]
    sink_logit = sink_logits.reshape(kv_heads, group_size)[None, :, :, None, None]
    masked = jnp.where(valid_pair, scores, -1e30)
    ceiling = jnp.maximum(jnp.max(masked, axis=-1, keepdims=True), sink_logit)
    weights = jnp.where(valid_pair, jnp.exp(masked - ceiling), 0.0)
    denominator = jnp.exp(sink_logit - ceiling) + jnp.sum(weights, axis=-1, keepdims=True)
    weights_bf = (weights / denominator).astype(jnp.bfloat16)
    mixed_rows = jnp.einsum(
        "khgij,kjhd->kihgd", weights_bf, value_band, preferred_element_type=jnp.float32
    )
    return mixed_rows.reshape(row_count, query_heads * head_dim).astype(jnp.bfloat16)


def block_terms(query_rows, key_rows, value_rows, log_rows, block_len):
    row_count, group_count, state_size = query_rows.shape
    head_ratio, head_dim = (value_rows.shape[2], value_rows.shape[3])
    block_count = row_count // block_len
    query_blocks = query_rows.reshape(block_count, block_len, group_count, state_size)
    key_blocks = key_rows.reshape(block_count, block_len, group_count, state_size)
    value_blocks = value_rows.reshape(block_count, block_len, group_count, head_ratio, head_dim)
    decay_cum = jnp.cumsum(
        log_rows.reshape(block_count, block_len, group_count, head_ratio), axis=1
    )
    decay_total = decay_cum[:, -1]
    gram_block = jnp.einsum(
        "kign,kjgn->kgij", query_blocks, key_blocks, preferred_element_type=jnp.float32
    )
    cum_heads = jnp.moveaxis(decay_cum, 1, 3)
    distance = jnp.abs(cum_heads[..., :, None] - cum_heads[..., None, :])
    pair_weight = (gram_block[:, :, None] * jnp.exp(-distance)).astype(jnp.bfloat16)
    near_terms = jnp.einsum(
        "kgrij,kjgrp->kigrp", pair_weight, value_blocks, preferred_element_type=jnp.float32
    )
    keys_after = (
        key_blocks[:, :, :, None, :] * jnp.exp(decay_total[:, None] - decay_cum)[..., None]
    ).astype(jnp.bfloat16)
    keys_before = (key_blocks[:, :, :, None, :] * jnp.exp(decay_cum)[..., None]).astype(
        jnp.bfloat16
    )
    state_after = jnp.einsum(
        "kjgrn,kjgrp->kgrnp", keys_after, value_blocks, preferred_element_type=jnp.float32
    )
    state_before = jnp.einsum(
        "kjgrn,kjgrp->kgrnp", keys_before, value_blocks, preferred_element_type=jnp.float32
    )
    before = jnp.cumsum(decay_total, axis=0) - decay_total
    overall = jnp.sum(decay_total, axis=0)
    after_sum = overall[None] - before - decay_total
    block_order = jnp.arange(block_count)
    earlier_mask = (block_order[None, :] < block_order[:, None])[:, :, None, None]
    later_mask = (block_order[None, :] > block_order[:, None])[:, :, None, None]
    gap_fwd = before[:, None] - before[None, :] - decay_total[None, :]
    gap_bwd = before[None, :] - before[:, None] - decay_total[:, None]
    weight_fwd = jnp.where(earlier_mask, jnp.exp(jnp.minimum(gap_fwd, 0.0)), 0.0)
    weight_bwd = jnp.where(later_mask, jnp.exp(jnp.minimum(gap_bwd, 0.0)), 0.0)
    carried_fwd = jnp.einsum(
        "abgr,bgrnp->agrnp", weight_fwd, state_after, precision=lax.Precision.HIGHEST
    )
    carried_bwd = jnp.einsum(
        "abgr,bgrnp->agrnp", weight_bwd, state_before, precision=lax.Precision.HIGHEST
    )
    summary_fwd = jnp.einsum(
        "agr,agrnp->grnp", jnp.exp(after_sum), state_after, precision=lax.Precision.HIGHEST
    )
    summary_bwd = jnp.einsum(
        "agr,agrnp->grnp", jnp.exp(before), state_before, precision=lax.Precision.HIGHEST
    )
    pieces = (
        near_terms,
        carried_fwd,
        carried_bwd,
        decay_cum,
        decay_total,
        before,
        after_sum,
        query_blocks,
    )
    return (pieces, (summary_fwd, summary_bwd, overall))


def finish_terms(pieces, incoming_fwd, incoming_bwd):
    (
        near_terms,
        carried_fwd,
        carried_bwd,
        decay_cum,
        decay_total,
        before,
        after_sum,
        query_blocks,
    ) = pieces
    total_fwd = carried_fwd + jnp.exp(before)[..., None, None] * incoming_fwd[None]
    total_bwd = carried_bwd + jnp.exp(after_sum)[..., None, None] * incoming_bwd[None]
    query_wide = query_blocks.astype(jnp.float32)
    read_fwd = jnp.einsum(
        "kign,kgrnp->kigrp", query_wide, total_fwd, precision=lax.Precision.HIGHEST
    )
    read_bwd = jnp.einsum(
        "kign,kgrnp->kigrp", query_wide, total_bwd, precision=lax.Precision.HIGHEST
    )
    combined = (
        near_terms
        + jnp.exp(decay_cum)[..., None] * read_fwd
        + jnp.exp(decay_total[:, None] - decay_cum)[..., None] * read_bwd
    )
    block_count, block_len, group_count, head_ratio, head_dim = combined.shape
    return combined.reshape(block_count * block_len, group_count, head_ratio, head_dim)


def combine_all(gathered_states, own_index):
    after_all, before_all, logs_all = gathered_states
    device_count = logs_all.shape[0]
    cum_incl = jnp.cumsum(logs_all, axis=0)
    cum_excl = cum_incl - logs_all
    device_order = jnp.arange(device_count)
    picker = (device_order == own_index).astype(jnp.float32)[:, None, None]
    own_incl = jnp.sum(picker * cum_incl, axis=0)
    own_excl = jnp.sum(picker * cum_excl, axis=0)
    lower_mask = (device_order < own_index)[:, None, None]
    higher_mask = (device_order > own_index)[:, None, None]
    weight_fwd = jnp.where(lower_mask, jnp.exp(jnp.minimum(own_excl[None] - cum_incl, 0.0)), 0.0)
    weight_bwd = jnp.where(higher_mask, jnp.exp(jnp.minimum(cum_excl - own_incl[None], 0.0)), 0.0)
    incoming_fwd = jnp.einsum(
        "dgr,dgrnp->grnp", weight_fwd, after_all, precision=lax.Precision.HIGHEST
    )
    incoming_bwd = jnp.einsum(
        "dgr,dgrnp->grnp", weight_bwd, before_all, precision=lax.Precision.HIGHEST
    )
    return (incoming_fwd, incoming_bwd)


def shards(
    tokens,
    norm_gain,
    state_gate,
    state_value,
    state_keys,
    state_query,
    state_step,
    state_rate,
    state_jumps,
    state_gain,
    filter_value,
    filter_keys,
    filter_query,
    window_query,
    window_keys,
    window_values,
    window_sink,
    state_output,
    window_output,
):
    row_count = tokens.shape[0]
    rows_wide = tokens.astype(jnp.float32)
    normed = (
        rows_wide
        * lax.rsqrt(jnp.mean(rows_wide * rows_wide, axis=-1, keepdims=True) + 1e-06)
        * norm_gain
    ).astype(jnp.bfloat16)
    gathered = (
        lax.all_gather(state_gate, "sp", axis=0, tiled=True),
        lax.all_gather(state_value, "sp", axis=0, tiled=True),
        lax.all_gather(state_keys, "sp", axis=0, tiled=True),
        lax.all_gather(state_query, "sp", axis=0, tiled=True),
        lax.all_gather(window_query, "sp", axis=0, tiled=True),
        lax.all_gather(window_keys, "sp", axis=0, tiled=True),
        lax.all_gather(window_values, "sp", axis=0, tiled=True),
        lax.all_gather(state_output, "sp", axis=1, tiled=True),
        lax.all_gather(window_output, "sp", axis=1, tiled=True),
    )
    projected = [
        jnp.dot(normed, matrix, preferred_element_type=jnp.float32) for matrix in gathered[:7]
    ]
    out_state = gathered[7]
    out_window = gathered[8]
    gate_rows, value_pre, keys_pre, query_pre, query_raw, keys_raw, values_rows = [
        result.astype(jnp.bfloat16) for result in projected
    ]
    head_local = state_rate.shape[0]
    group_local = keys_pre.shape[1] // STATE_SIZE
    head_dim = value_pre.shape[1] // head_local
    head_ratio = head_local // group_local
    step_cols = lax.dynamic_slice_in_dim(
        state_step, lax.axis_index("tp") * head_local, head_local, 1
    )
    step_rows = jax.nn.softplus(jnp.dot(normed, step_cols, preferred_element_type=jnp.float32))
    log_decay = -state_rate[None, :] * step_rows + state_jumps
    half_width = filter_value.shape[0] // 2
    stacked = jnp.concatenate([value_pre, keys_pre, query_pre], axis=-1)
    padded = extended(stacked, (("sp", 0),), half_width)
    filters = jnp.concatenate([filter_value, filter_keys, filter_query], axis=-1).astype(
        jnp.float32
    )
    filtered = jnp.zeros(stacked.shape, jnp.float32)
    for offset in range(filters.shape[0]):
        filtered = (
            filtered + padded[offset : offset + row_count].astype(jnp.float32) * filters[offset]
        )
    value_cols = value_pre.shape[1]
    key_cols = keys_pre.shape[1]
    inner_rows = (
        jax.nn.silu(filtered[:, :value_cols]).reshape(row_count, head_local, head_dim)
        * step_rows[..., None]
    )
    scan_values = inner_rows.astype(jnp.bfloat16).reshape(
        row_count, group_local, head_ratio, head_dim
    )
    scan_keys = (
        filtered[:, value_cols : value_cols + key_cols]
        .astype(jnp.bfloat16)
        .reshape(row_count, group_local, STATE_SIZE)
    )
    scan_query = (
        filtered[:, value_cols + key_cols :]
        .astype(jnp.bfloat16)
        .reshape(row_count, group_local, STATE_SIZE)
    )
    pieces, summaries = block_terms(
        scan_query,
        scan_keys,
        scan_values,
        log_decay.reshape(row_count, group_local, head_ratio),
        BLOCK,
    )
    summary_fwd, summary_bwd, overall = summaries
    gathered_states = (
        lax.all_gather(summary_fwd[None].astype(jnp.bfloat16), "sp", axis=0, tiled=True).astype(
            jnp.float32
        ),
        lax.all_gather(summary_bwd[None].astype(jnp.bfloat16), "sp", axis=0, tiled=True).astype(
            jnp.float32
        ),
        lax.all_gather(overall[None].astype(jnp.bfloat16), "sp", axis=0, tiled=True).astype(
            jnp.float32
        ),
    )
    incoming_fwd, incoming_bwd = combine_all(gathered_states, lax.axis_index("sp"))
    scan_out = finish_terms(pieces, incoming_fwd, incoming_bwd).reshape(
        row_count, head_local * head_dim
    )
    gated_rows = scan_out * jax.nn.silu(gate_rows.astype(jnp.float32))
    per_head = gated_rows.reshape(row_count, head_local, head_dim)
    state_mix = (
        (
            per_head
            * lax.rsqrt(jnp.mean(per_head * per_head, axis=-1, keepdims=True) + 1e-06)
            * state_gain.reshape(head_local, head_dim)
        )
        .astype(jnp.bfloat16)
        .reshape(row_count, head_local * head_dim)
    )
    query_heads = window_sink.shape[0]
    kv_heads = keys_raw.shape[1] // HEAD_DIM
    kv_width = kv_heads * HEAD_DIM
    positions = lax.axis_index("sp") * row_count + jnp.arange(row_count, dtype=jnp.int32)
    query_rot = rotate_grid(
        query_raw.reshape(row_count, query_heads, HEAD_DIM), positions, GRID_WIDTH
    )
    keys_rot = rotate_grid(keys_raw.reshape(row_count, kv_heads, HEAD_DIM), positions, GRID_WIDTH)
    pair_rows = jnp.concatenate([keys_rot.reshape(row_count, kv_width), values_rows], axis=-1)
    padded_pair = extended(pair_rows, (("sp", 0),), WINDOW)
    keys_pad = padded_pair[:, :kv_width].reshape(-1, kv_heads, HEAD_DIM)
    values_pad = padded_pair[:, kv_width:].reshape(-1, kv_heads, HEAD_DIM)
    window_mix = window_attend(
        query_rot,
        keys_pad,
        values_pad,
        window_sink,
        lax.axis_index("sp") * row_count - WINDOW,
        lax.axis_size("sp") * row_count,
        WINDOW,
    )
    return lax.psum_scatter(
        (
            jnp.dot(state_mix, out_state, preferred_element_type=jnp.float32)
            + jnp.dot(window_mix, out_window, preferred_element_type=jnp.float32)
        ).astype(jnp.bfloat16),
        "tp",
        scatter_dimension=0,
        tiled=True,
    )


def own_part(array, axis, dim):
    size = array.shape[dim] // lax.axis_size(axis)
    return lax.dynamic_slice_in_dim(array, lax.axis_index(axis) * size, size, dim)


def line_kernel(count, block_ref, out_ref, own_sem, send_up, recv_up, send_down, recv_down):
    me = lax.axis_index("sp")
    barrier = pltpu.get_barrier_semaphore()
    has_left, has_right = me > 0, me < count - 1
    left, right = jnp.maximum(me - 1, 0), jnp.minimum(me + 1, count - 1)

    def greet(other):
        pl.semaphore_signal(
            barrier, inc=1, device_id={"sp": other}, device_id_type=pl.DeviceIdType.MESH
        )

    pl.when(has_left)(lambda: greet(left))
    pl.when(has_right)(lambda: greet(right))
    pl.semaphore_wait(barrier, jnp.minimum(me, 1) + jnp.minimum(count - 1 - me, 1))

    def passing(hop, origin, other, send_sems, recv_sems):
        return pltpu.make_async_remote_copy(
            src_ref=block_ref if hop == 0 else out_ref.at[origin],
            dst_ref=out_ref.at[origin],
            send_sem=send_sems.at[hop],
            recv_sem=recv_sems.at[hop],
            device_id={"sp": other},
            device_id_type=pl.DeviceIdType.MESH,
        )

    def up(hop):
        return passing(hop, jnp.maximum(me - hop, 0), right, send_up, recv_up)

    def down(hop):
        return passing(hop, jnp.minimum(me + hop, count - 1), left, send_down, recv_down)

    own = pltpu.make_async_copy(block_ref, out_ref.at[me], own_sem)
    for hop in range(count):
        if hop >= 1:
            pl.when(me >= hop)(lambda: up(hop - 1).wait_recv())
        if hop < count - 1:
            pl.when(has_right & (me >= hop))(lambda: up(hop).start())
        if hop >= 1:
            pl.when(me + hop <= count - 1)(lambda: down(hop - 1).wait_recv())
        if hop < count - 1:
            pl.when(has_left & (me + hop <= count - 1))(lambda: down(hop).start())
        if hop == 0:
            own.start()
    for hop in range(count - 1):
        pl.when(has_right & (me >= hop))(lambda: up(hop).wait_send())
        pl.when(has_left & (me + hop <= count - 1))(lambda: down(hop).wait_send())
    own.wait()


def line_gather(block):
    count = lax.axis_size("sp")
    size = block.size * block.dtype.itemsize * count
    return pl.pallas_call(
        functools.partial(line_kernel, count),
        out_shape=jax.ShapeDtypeStruct((count,) + block.shape, block.dtype),
        in_specs=[pl.BlockSpec(memory_space=pl.ANY)],
        out_specs=pl.BlockSpec(memory_space=pl.ANY),
        scratch_shapes=[pltpu.SemaphoreType.DMA] + [pltpu.SemaphoreType.DMA((count - 1,))] * 4,
        compiler_params=pltpu.CompilerParams(collective_id=0, has_side_effects=True),
        cost_estimate=pl.CostEstimate(flops=0, bytes_accessed=size * 40, transcendentals=0),
    )(block)


def carried_in(state, log, direction):
    count = lax.axis_size("sp")
    groups, ratio, size, width = state.shape
    lanes = ratio * width
    wide = jnp.moveaxis(state.astype(jnp.bfloat16), 1, 2).reshape(groups, size, lanes)
    high = log.astype(jnp.bfloat16)
    low = (log - high.astype(jnp.float32)).astype(jnp.bfloat16)
    rows = [
        jnp.broadcast_to(part[:, None, :, None], (groups, 8, ratio, width)).reshape(
            groups, 8, lanes
        )
        for part in (high, low)
    ]
    packed = jnp.concatenate([wide] + rows, axis=1)
    incoming, between = 0.0, None
    for hop in range(1, count):
        pairs = [(i, i + hop) for i in range(count - hop)]
        if direction < 0:
            pairs = [(j, i) for i, j in pairs]
        arrived = lax.ppermute(packed, "sp", pairs).astype(jnp.float32)
        share, passed = arrived[:, :size], arrived[:, size] + arrived[:, size + 8]
        incoming = share if between is None else incoming + jnp.exp(between)[:, None] * share
        between = passed if between is None else between + passed
    return jnp.moveaxis(incoming.reshape(groups, size, ratio, width), 2, 1)


def rotate_lanes(vectors, positions, grid_width):
    head_dim = vectors.shape[-1]
    quarter = head_dim // 4
    lane = jnp.arange(head_dim)
    inverse = 10000.0 ** (-(lane % quarter).astype(jnp.float32) / quarter)
    grid_row = (positions // grid_width).astype(jnp.float32)
    grid_col = (positions % grid_width).astype(jnp.float32)
    place = jnp.where((lane < 2 * quarter)[None, :], grid_row[:, None], grid_col[:, None])
    angles = (place * inverse[None, :])[:, None, :]
    lower = lane % (2 * quarter) < quarter
    source = jnp.where(lower, lane + quarter, lane - quarter)
    sign = jnp.where(lower, -1.0, 1.0)
    turn = jnp.where(lane[:, None] == source[None, :], sign[None, :], 0.0).astype(jnp.bfloat16)
    turned = jnp.einsum("thd,de->the", vectors, turn, preferred_element_type=jnp.float32)
    return (
        vectors.astype(jnp.float32) * jnp.cos(angles) + turned * jnp.sin(angles)
    ).astype(jnp.bfloat16)


def mixers(
    projected,
    step_rows,
    state_rate,
    state_jumps,
    state_gain,
    filters,
    window_sink,
    widths,
):
    row_count = projected.shape[0]
    pieces = []
    start = 0
    for width in widths:
        pieces.append(projected[:, start : start + width])
        start += width
    gate_rows, value_pre, keys_pre, query_pre, query_raw, keys_raw, values_rows = pieces
    stacked = projected[:, widths[0] : widths[0] + widths[1] + widths[2] + widths[3]]
    head_local = state_rate.shape[0]
    group_local = keys_pre.shape[1] // STATE_SIZE
    head_dim = value_pre.shape[1] // head_local
    head_ratio = head_local // group_local
    log_decay = -state_rate[None, :] * step_rows + state_jumps
    half_width = filters.shape[0] // 2
    padded = extended(stacked, (("sp", 0),), half_width)
    filtered = jnp.zeros(stacked.shape, jnp.float32)
    for offset in range(filters.shape[0]):
        filtered = (
            filtered + padded[offset : offset + row_count].astype(jnp.float32) * filters[offset]
        )
    value_cols = value_pre.shape[1]
    key_cols = keys_pre.shape[1]
    inner_rows = (
        jax.nn.silu(filtered[:, :value_cols]).reshape(row_count, head_local, head_dim)
        * step_rows[..., None]
    )
    scan_values = inner_rows.astype(jnp.bfloat16).reshape(
        row_count, group_local, head_ratio, head_dim
    )
    scan_keys = (
        filtered[:, value_cols : value_cols + key_cols]
        .astype(jnp.bfloat16)
        .reshape(row_count, group_local, STATE_SIZE)
    )
    scan_query = (
        filtered[:, value_cols + key_cols :]
        .astype(jnp.bfloat16)
        .reshape(row_count, group_local, STATE_SIZE)
    )
    pieces, summaries = block_terms(
        scan_query,
        scan_keys,
        scan_values,
        log_decay.reshape(row_count, group_local, head_ratio),
        BLOCK,
    )
    summary_fwd, summary_bwd, overall = summaries
    incoming_fwd = carried_in(summary_fwd, overall, 1)
    incoming_bwd = carried_in(summary_bwd, overall, -1)
    scan_out = finish_terms(pieces, incoming_fwd, incoming_bwd).reshape(
        row_count, head_local * head_dim
    )
    gated_rows = scan_out * jax.nn.silu(gate_rows.astype(jnp.float32))
    per_head = gated_rows.reshape(row_count, head_local, head_dim)
    state_mix = (
        (
            per_head
            * lax.rsqrt(jnp.mean(per_head * per_head, axis=-1, keepdims=True) + 1e-06)
            * state_gain.reshape(head_local, head_dim)
        )
        .astype(jnp.bfloat16)
        .reshape(row_count, head_local * head_dim)
    )
    query_heads = window_sink.shape[0]
    kv_heads = keys_raw.shape[1] // HEAD_DIM
    kv_width = kv_heads * HEAD_DIM
    positions = lax.axis_index("sp") * row_count + jnp.arange(row_count, dtype=jnp.int32)
    turning = projected[:, sum(widths[:4]) : sum(widths[:6])]
    turned = rotate_lanes(
        turning.reshape(row_count, query_heads + kv_heads, HEAD_DIM), positions, GRID_WIDTH
    )
    query_rot, keys_rot = turned[:, :query_heads], turned[:, query_heads:]
    pair_rows = jnp.concatenate([keys_rot.reshape(row_count, kv_width), values_rows], axis=-1)
    padded_pair = extended(pair_rows, (("sp", 0),), WINDOW)
    keys_pad = padded_pair[:, :kv_width].reshape(-1, kv_heads, HEAD_DIM)
    values_pad = padded_pair[:, kv_width:].reshape(-1, kv_heads, HEAD_DIM)
    window_mix = window_attend(
        query_rot,
        keys_pad,
        values_pad,
        window_sink,
        lax.axis_index("sp") * row_count - WINDOW,
        lax.axis_size("sp") * row_count,
        WINDOW,
    )
    return jnp.concatenate([state_mix, window_mix], axis=-1)


def split_shards(
    tokens,
    norm_gain,
    state_gate,
    state_value,
    state_keys,
    state_query,
    state_step,
    state_rate,
    state_jumps,
    state_gain,
    filter_value,
    filter_keys,
    filter_query,
    window_query,
    window_keys,
    window_values,
    window_sink,
    state_output,
    window_output,
):
    row_count = tokens.shape[0]
    parts = lax.axis_size("fs")
    weights = [
        own_part(matrix, "fs", 1)
        for matrix in (
            state_gate,
            state_value,
            state_keys,
            state_query,
            window_query,
            window_keys,
            window_values,
        )
    ]
    widths = tuple(matrix.shape[1] for matrix in weights)
    rows_wide = own_part(tokens, "tp", 0).astype(jnp.float32)
    normed_own = (
        rows_wide
        * lax.rsqrt(jnp.mean(rows_wide * rows_wide, axis=-1, keepdims=True) + 1e-06)
        * norm_gain
    ).astype(jnp.bfloat16)
    out_rows = jnp.concatenate(
        [own_part(state_output, "fs", 0), own_part(window_output, "fs", 0)], axis=0
    )
    out_all = lax.all_gather(out_rows, ("sp", "fs"), axis=0, tiled=True)
    block, normed_own = lax.optimization_barrier((jnp.concatenate(weights, axis=1), normed_own))
    normed = lax.all_gather(normed_own, ("fs", "tp"), axis=0, tiled=True)
    matrix = line_gather(block)
    total = jnp.dot(
        normed, matrix.reshape(-1, block.shape[1]), preferred_element_type=jnp.float32
    )
    projected = total.astype(jnp.bfloat16).reshape(parts, row_count, -1)
    heads = state_rate.shape[0] // parts
    first = lax.axis_index("tp") * state_rate.shape[0] + lax.axis_index("fs") * heads
    step_cols = lax.dynamic_slice_in_dim(state_step, first, heads, 1)
    step_rows = jax.nn.softplus(jnp.dot(normed, step_cols, preferred_element_type=jnp.float32))
    jumps = lax.all_to_all(
        state_jumps.reshape(row_count, parts, heads), "fs", split_axis=1, concat_axis=0
    )
    filters = jnp.concatenate(
        [own_part(taps, "fs", 1) for taps in (filter_value, filter_keys, filter_query)], axis=-1
    ).astype(jnp.float32)
    rate = own_part(state_rate, "fs", 0)
    gain = own_part(state_gain, "fs", 0)
    sink = own_part(window_sink, "fs", 0)
    mix = jax.vmap(
        lambda rows, steps, jump: mixers(rows, steps, rate, jump, gain, filters, sink, widths)
    )(projected, step_rows.reshape(parts, row_count, heads), jumps.reshape(parts, row_count, heads))
    mix = lax.all_to_all(mix, "fs", split_axis=0, concat_axis=0, tiled=True)
    mix = jnp.moveaxis(mix, 0, 1).reshape(row_count, -1)
    out_all = out_all.reshape(lax.axis_size("sp"), mix.shape[1], -1)
    shares = jnp.concatenate(
        [
            jnp.dot(mix, out_all[i], preferred_element_type=jnp.float32).astype(jnp.bfloat16)
            for i in range(out_all.shape[0])
        ],
        axis=1,
    )
    return lax.psum_scatter(shares, "tp", scatter_dimension=0, tiled=True)


def solution(mesh):
    placed = (
        P(("fs", "sp"), None),
        P(),
        P("sp", "tp"),
        P("sp", "tp"),
        P("sp", "tp"),
        P("sp", "tp"),
        P(),
        P("tp"),
        P(("fs", "sp"), "tp"),
        P("tp"),
        P(None, "tp"),
        P(None, "tp"),
        P(None, "tp"),
        P("sp", "tp"),
        P("sp", "tp"),
        P("sp", "tp"),
        P("tp"),
        P("tp", "sp"),
        P("tp", "sp"),
    )
    def plan(*args):
        parts = lax.axis_size("fs")
        groups = args[4].shape[1] // STATE_SIZE
        kv_heads = args[14].shape[1] // HEAD_DIM
        even = groups % parts == 0 and kv_heads % parts == 0
        return (split_shards if even else shards)(*args)

    return jax.shard_map(
        plan, mesh=mesh, in_specs=placed, out_specs=P(("fs", "sp", "tp"), None), check_vma=False
    )
```
